32 devices in a mesh: rep: 2 (over x), fs: 8 (over z, y), tp: 2 (over core).
Axes of the slice: x: 2, y: 2, z: 4, core: 2. Of those that a mesh axis runs over, the one named last changes fastest.
Arguments:
- tokens: bfloat16 [16384, 2048], P(('rep', 'fs'), 'tp'), may hold values from -6 to 6
- attention_pre_gain: float32 [2048], replicated, may hold values from 0.1 to 1.9
- query_matrix: bfloat16 [2048, 512], P('fs', 'tp'), may hold values from -0.125 to 0.125
- key_matrix: bfloat16 [2048, 512], P('fs', 'tp'), may hold values from -0.125 to 0.125
- value_matrix: bfloat16 [2048, 1024], P('fs', 'tp'), may hold values from -0.125 to 0.125
- decay_first_weight: bfloat16 [2048, 16], replicated, may hold values from -0.125 to 0.125
- decay_second_weight: bfloat16 [16, 512], P(None, 'tp'), may hold values from -1.5 to 1.5
- decay_offset_bias: float32 [512], P('tp'), may hold values from 0 to 6
- extra_log_surge: float32 [16384, 2], P(('rep', 'fs'), 'tp'), may hold values from -0.7 to 0
- readout_head_gain: float32 [512], replicated, may hold values from 0.1 to 1.9
- output_matrix: bfloat16 [1024, 2048], P('tp', 'fs'), may hold values from -2.4375 to 2.4375
- attention_post_gain: float32 [2048], P('tp'), may hold values from 0.1 to 1.9
- feedforward_pre_gain: float32 [2048], replicated, may hold values from 0.1 to 1.9
- up_matrix: bfloat16 [2048, 4096], P('fs', 'tp'), may hold values from -0.125 to 0.125
- down_matrix: bfloat16 [4096, 2048], P('tp', 'fs'), may hold values from -1.21875 to 1.21875
- feedforward_post_gain: float32 [2048], P('tp'), may hold values from 0.1 to 1.9
Outputs:
- layer_out: bfloat16 [16384, 2048], P(('rep', 'fs'), 'tp')
The draws below stay inside these ranges and needn't reach their ends.
All inputs are finite; a program needn't handle non-finite values.
Results may differ from the reference program's by a relative error of at most 0.017.
Values may be sent and summed in bfloat16 or wider, within the bound.
A program may use at most 128 MiB of HBM per device.

```python
import jax
import jax.numpy as jnp
from jax import lax

D = 2048
FF = 4096
HEADS = 2
KEY_WIDTH = 256
DV = 512
RANK = 16
BLOCK = 64
LENGTH = 1024
KEYDIM = 512
VALDIM = 1024
TOKENS = 16384
N_TP = 2


def draw_decay_offset_bias(key, part):
    base = jax.random.fold_in(key, 11)
    first, second, third = jax.random.split(base, 3)
    slow_share = 0.5
    chosen = jax.random.uniform(first, (KEYDIM,), jnp.float32) < slow_share
    slow_value = jax.random.uniform(second, (KEYDIM,), jnp.float32, 4.0, 6.0)
    fast_value = jax.random.uniform(third, (KEYDIM,), jnp.float32, 0.0, 1.5)
    return jnp.where(chosen, slow_value, fast_value)


def draw_extra_log_surge(key, part):
    base = jax.random.fold_in(key, 23)
    first, second = jax.random.split(base, 2)
    marked = jax.random.randint(first, (TOKENS, HEADS), 0, LENGTH // 4) == 0
    sizes = jnp.log(jax.random.uniform(second, (TOKENS, HEADS), jnp.float32, 0.5, 0.8))
    return jnp.where(marked, sizes, jnp.zeros((TOKENS, HEADS), jnp.float32))


def ramped_matrix(key, rows, columns):
    first, second = jax.random.split(key, 2)
    entries = jnp.clip(jax.random.normal(first, (rows, columns), jnp.float32), -6.0, 6.0)
    top_scale = 10.0
    ramp = jnp.exp(jnp.log(top_scale) * jnp.arange(columns, dtype=jnp.float32) / columns)
    rough = jax.random.uniform(second, (columns,), jnp.float32, 0.7, 1.3)
    return (entries * rows ** (-0.5) * (ramp * rough)[None, :]).astype(jnp.bfloat16)


def draw_down_matrix(key, part):
    return ramped_matrix(jax.random.fold_in(key, 37), FF, D)


def draw_output_matrix(key, part):
    return ramped_matrix(jax.random.fold_in(key, 53), VALDIM, D)


def shard_levels(key, dims, pieces, low, high):
    factor_of, own = 1.0, jax.random.fold_in(key, 6)
    for position, parts in pieces:
        draws = jnp.exp(jax.random.uniform(jax.random.fold_in(own, position), (parts,), jnp.float32, low / len(pieces), high / len(pieces)))
        factor_of = factor_of * jnp.repeat(draws, dims[position] // parts).reshape([-1 if axis == position else 1 for axis in range(len(dims))])
    return factor_of


def bell_draw(stream_key, shape, deviation, limit, cuts=(), held_as=jnp.bfloat16):
    drawn = jax.random.normal(stream_key, shape, jnp.float32) * deviation
    if len(cuts) > 0:
        drawn = shard_levels(stream_key, shape, cuts, -0.22, 0.18) * drawn
    return jnp.clip(drawn, min=-limit, max=limit).astype(held_as)


def setup_inputs(seed: int = 0) -> dict:
    key_of = jax.random.split(jax.random.key(seed), 17)
    tokens = bell_draw(key_of[0], (TOKENS, D), 1.0, 6.0, ((0, 16), (1, 2)))
    attention_pre_gain = jnp.clip(1.0 + 0.18 * jax.random.normal(key_of[1], (D,), jnp.float32), 0.1, 1.9)
    query_matrix = bell_draw(key_of[2], (D, KEYDIM), D ** -0.5, 0.125, ((0, 8), (1, 2)))
    key_matrix = bell_draw(key_of[3], (D, KEYDIM), D ** -0.5, 0.125, ((0, 8), (1, 2)))
    value_matrix = bell_draw(key_of[4], (D, VALDIM), D ** -0.5, 0.125, ((0, 8), (1, 2)))
    decay_first_weight = bell_draw(key_of[5], (D, RANK), D ** -0.5, 0.125)
    decay_second_weight = bell_draw(key_of[6], (RANK, KEYDIM), RANK ** -0.5, 1.5, ((1, 2),))
    decay_offset_bias = draw_decay_offset_bias(jax.random.fold_in(key_of[16], 71), 0)
    extra_log_surge = draw_extra_log_surge(jax.random.fold_in(key_of[16], 71), 0)
    readout_head_gain = jnp.clip(1.0 + 0.18 * jax.random.normal(key_of[9], (DV,), jnp.float32), 0.1, 1.9)
    output_matrix = draw_output_matrix(jax.random.fold_in(key_of[16], 71), 0)
    attention_post_gain = jnp.clip(1.0 + 0.18 * jax.random.normal(key_of[11], (D,), jnp.float32), 0.1, 1.9)
    feedforward_pre_gain = jnp.clip(1.0 + 0.18 * jax.random.normal(key_of[12], (D,), jnp.float32), 0.1, 1.9)
    up_matrix = bell_draw(key_of[13], (D, FF), D ** -0.5, 0.125, ((0, 8), (1, 2)))
    down_matrix = draw_down_matrix(jax.random.fold_in(key_of[16], 71), 0)
    feedforward_post_gain = jnp.clip(1.0 + 0.18 * jax.random.normal(key_of[15], (D,), jnp.float32), 0.1, 1.9)
    return {"tokens": tokens, "attention_pre_gain": attention_pre_gain, "query_matrix": query_matrix, "key_matrix": key_matrix, "value_matrix": value_matrix, "decay_first_weight": decay_first_weight, "decay_second_weight": decay_second_weight, "decay_offset_bias": decay_offset_bias, "extra_log_surge": extra_log_surge, "readout_head_gain": readout_head_gain, "output_matrix": output_matrix, "attention_post_gain": attention_post_gain, "feedforward_pre_gain": feedforward_pre_gain, "up_matrix": up_matrix, "down_matrix": down_matrix, "feedforward_post_gain": feedforward_post_gain}


EPS = 1e-06

def pre_norm(rows, gain):
    values = rows.astype(jnp.float32)
    scale = lax.rsqrt(lax.optimization_barrier(jnp.mean(values * values, axis=-1, keepdims=True)) + EPS)
    return (values * scale * gain).astype(jnp.bfloat16)

def block_attention(queries, keys_in, values_in, log_gates):
    head_count, token_length, key_size = queries.shape
    value_size = values_in.shape[-1]
    blocks = token_length // BLOCK

    def to_blocks(array):
        return array.reshape(head_count, blocks, BLOCK, array.shape[-1]).transpose(1, 0, 2, 3)
    causal = jnp.tril(jnp.ones((BLOCK, BLOCK), dtype=bool))[None, :, :, None]
    highest = lax.Precision.HIGHEST

    def advance(memory_state, inputs):
        query_blk, key_blk, value_blk, gate_blk = inputs
        cumulative = jnp.cumsum(gate_blk, axis=1)
        carried = jnp.einsum('hid,hde->hie', query_blk * jnp.exp(cumulative), memory_state, precision=highest)
        spread_log = cumulative[:, :, None, :] - cumulative[:, None, :, :]
        weights = jnp.exp(jnp.where(causal, spread_log, -jnp.inf))
        scores = jnp.einsum('hid,hjd,hijd->hij', query_blk, key_blk, weights, precision=highest)
        readout = carried + jnp.einsum('hij,hje->hie', scores, value_blk, precision=highest)
        final_log = cumulative[:, -1:, :]
        memory_state = jnp.exp(final_log[:, 0, :])[:, :, None] * memory_state + jnp.einsum('hjd,hje->hde', key_blk * jnp.exp(final_log - cumulative), value_blk, precision=highest)
        return (memory_state, readout)
    start_state = jnp.zeros((head_count, key_size, value_size), jnp.float32)
    _, readout = lax.scan(advance, start_state, (to_blocks(queries), to_blocks(keys_in), to_blocks(values_in), to_blocks(log_gates)))
    return readout.transpose(1, 0, 2, 3).reshape(head_count, token_length, value_size)

def grouped_sum(left, right):
    group = left.shape[1] // N_TP
    total = jnp.zeros((left.shape[0], right.shape[1]), jnp.float32)
    for member in range(N_TP):
        partial_value = jnp.dot(left[:, member * group:(member + 1) * group], right[member * group:(member + 1) * group], preferred_element_type=jnp.float32)
        rounded = lax.optimization_barrier(partial_value.astype(jnp.bfloat16))
        total = total + rounded.astype(jnp.float32)
    return total

def post_add(resid, branch, gain):
    scale = lax.rsqrt(lax.optimization_barrier(jnp.mean(branch * branch, axis=-1, keepdims=True)) + EPS)
    return (resid.astype(jnp.float32) + branch * scale * gain).astype(jnp.bfloat16)

def reference(tokens, attention_pre_gain, query_matrix, key_matrix, value_matrix, decay_first_weight, decay_second_weight, decay_offset_bias, extra_log_surge, readout_head_gain, output_matrix, attention_post_gain, feedforward_pre_gain, up_matrix, down_matrix, feedforward_post_gain):
    normed = pre_norm(tokens, attention_pre_gain)
    query_proj = jnp.dot(normed, query_matrix, preferred_element_type=jnp.float32).astype(jnp.bfloat16)
    key_proj = jnp.dot(normed, key_matrix, preferred_element_type=jnp.float32).astype(jnp.bfloat16)
    value_proj = jnp.dot(normed, value_matrix, preferred_element_type=jnp.float32).astype(jnp.bfloat16)
    rank_rows = jnp.dot(normed, decay_first_weight, preferred_element_type=jnp.float32).astype(jnp.bfloat16)
    gate_source_input = jnp.dot(rank_rows, decay_second_weight, preferred_element_type=jnp.float32) + decay_offset_bias
    logarithm_decay = jax.nn.log_sigmoid(gate_source_input) / 16.0 + jnp.repeat(extra_log_surge, KEY_WIDTH, axis=1)
    sequences = TOKENS // LENGTH

    def by_head(array, size):
        return array.astype(jnp.float32).reshape(sequences, LENGTH, HEADS, size).transpose(0, 2, 1, 3)
    queries = by_head(query_proj, KEY_WIDTH) * KEY_WIDTH ** (-0.5)
    readout = lax.map(lambda group: block_attention(*group), (queries, by_head(key_proj, KEY_WIDTH), by_head(value_proj, DV), by_head(logarithm_decay, KEY_WIDTH)))
    readout = readout.transpose(0, 2, 1, 3).reshape(TOKENS, HEADS, DV)
    head_scale = lax.rsqrt(lax.optimization_barrier(jnp.mean(readout * readout, axis=-1, keepdims=True)) + EPS)
    mixed = (readout * head_scale * readout_head_gain).astype(jnp.bfloat16).reshape(TOKENS, VALDIM)
    attn = grouped_sum(mixed, output_matrix)
    resid = post_add(tokens, attn, attention_post_gain)
    normed_mid = pre_norm(resid, feedforward_pre_gain)
    hidden = jax.nn.relu(jnp.dot(normed_mid, up_matrix, preferred_element_type=jnp.float32))
    squared = (hidden * hidden).astype(jnp.bfloat16)
    feed = grouped_sum(squared, down_matrix)
    return post_add(resid, feed, feedforward_post_gain)
```

```python
import functools

import jax
import jax.numpy as jnp
from jax import lax
from jax.experimental import pallas as pl
from jax.experimental.pallas import tpu as pltpu
from jax.sharding import PartitionSpec as P

KEY_WIDTH = 256
DV = 512
LENGTH = 1024
CHUNK = 128
SUB = 16
EPS = 1e-06


def pre_norm(rows, gain):
    values = rows.astype(jnp.float32)
    scale = lax.rsqrt(jnp.mean(values * values, axis=-1, keepdims=True) + EPS)
    return (values * scale * gain).astype(jnp.bfloat16)


def attention_kernel(
    q_ref, k_ref, v_ref, rank_ref, second_ref, bias_ref, surge_ref, gain_ref, o_ref, state
):
    subs = CHUNK // SUB

    @pl.when(lax.rem(pl.program_id(1), LENGTH // CHUNK) == 0)
    def _():
        state[...] = jnp.zeros_like(state)

    q = q_ref[...].astype(jnp.float32) * KEY_WIDTH ** (-0.5)
    k = k_ref[...].astype(jnp.float32)
    v = v_ref[...]
    source = (
        jnp.dot(rank_ref[...], second_ref[...], preferred_element_type=jnp.float32)
        + bias_ref[...]
    )
    log_sig = jnp.minimum(source, 0.0) - jnp.log1p(jnp.exp(-jnp.abs(source)))
    gate = log_sig / 16.0 + surge_ref[0]

    row = lax.broadcasted_iota(jnp.int32, (CHUNK, CHUNK), 0)
    col = lax.broadcasted_iota(jnp.int32, (CHUNK, CHUNK), 1)
    lower = (row >= col).astype(jnp.float32)
    cum = jnp.dot(
        lower, gate, preferred_element_type=jnp.float32, precision=lax.Precision.HIGHEST
    )

    q3 = q.reshape(subs, SUB, KEY_WIDTH)
    k3 = k.reshape(subs, SUB, KEY_WIDTH)
    c3 = cum.reshape(subs, SUB, KEY_WIDTH)
    pick_col = lax.rem(lax.broadcasted_iota(jnp.int32, (KEY_WIDTH, CHUNK), 1), SUB)
    scores = jnp.zeros((CHUNK, CHUNK), jnp.float32)
    for j in range(SUB):
        weight = jnp.exp(jnp.minimum(c3 - c3[:, j : j + 1, :], 0.0))
        term = (q3 * k3[:, j : j + 1, :] * weight).reshape(CHUNK, KEY_WIDTH)
        scores += jnp.dot(
            term.astype(jnp.bfloat16),
            (pick_col == j).astype(jnp.bfloat16),
            preferred_element_type=jnp.float32,
        )
    scores = jnp.where((row // SUB == col // SUB) & (row >= col), scores, 0.0)

    pieces = [jnp.zeros((SUB, CHUNK), jnp.float32)]
    key_row = lax.broadcasted_iota(jnp.int32, (CHUNK, KEY_WIDTH), 0)
    for i in range(1, subs):
        edge = cum[i * SUB - 1 : i * SUB, :]
        left = q3[i] * jnp.exp(jnp.minimum(c3[i] - edge, 0.0))
        right = jnp.where(key_row < i * SUB, k * jnp.exp(jnp.minimum(edge - cum, 0.0)), 0.0)
        pieces.append(
            lax.dot_general(
                left.astype(jnp.bfloat16),
                right.astype(jnp.bfloat16),
                (((1,), (1,)), ((), ())),
                preferred_element_type=jnp.float32,
            )
        )
    scores = scores + jnp.concatenate(pieces, axis=0)

    last = cum[CHUNK - 1 : CHUNK, :]
    held = state[...]
    readout = lax.dot_general(
        (q * jnp.exp(cum)).astype(jnp.bfloat16),
        held.astype(jnp.bfloat16),
        (((1,), (1,)), ((), ())),
        preferred_element_type=jnp.float32,
    ) + jnp.dot(scores.astype(jnp.bfloat16), v, preferred_element_type=jnp.float32)
    faded = (k * jnp.exp(jnp.minimum(last - cum, 0.0))).astype(jnp.bfloat16)
    state[...] = held * jnp.exp(last) + lax.dot_general(
        v, faded, (((0,), (0,)), ((), ())), preferred_element_type=jnp.float32
    )
    scale = lax.rsqrt(jnp.mean(readout * readout, axis=-1, keepdims=True) + EPS)
    o_ref[...] = (readout * scale * gain_ref[...]).astype(jnp.bfloat16)


def attention(qkv, rank_rows, second, bias, surge, gain):
    tokens = qkv.shape[0]
    heads = second.shape[1] // KEY_WIDTH
    rank = rank_rows.shape[1]
    value_base = 2 * heads * KEY_WIDTH // DV
    return pl.pallas_call(
        attention_kernel,
        grid=(heads, tokens // CHUNK),
        in_specs=[
            pl.BlockSpec((CHUNK, KEY_WIDTH), lambda h, c: (c, h)),
            pl.BlockSpec((CHUNK, KEY_WIDTH), lambda h, c: (c, heads + h)),
            pl.BlockSpec((CHUNK, DV), lambda h, c: (c, value_base + h)),
            pl.BlockSpec((CHUNK, rank), lambda h, c: (c, 0)),
            pl.BlockSpec((rank, KEY_WIDTH), lambda h, c: (0, h)),
            pl.BlockSpec((1, KEY_WIDTH), lambda h, c: (0, h)),
            pl.BlockSpec((1, CHUNK, 1), lambda h, c: (h, c, 0)),
            pl.BlockSpec((1, DV), lambda h, c: (0, 0)),
        ],
        out_specs=pl.BlockSpec((CHUNK, DV), lambda h, c: (c, h)),
        out_shape=jax.ShapeDtypeStruct((tokens, heads * DV), jnp.bfloat16),
        scratch_shapes=[pltpu.VMEM((DV, KEY_WIDTH), jnp.float32)],
        compiler_params=pltpu.CompilerParams(
            dimension_semantics=("arbitrary", "arbitrary"), vmem_limit_bytes=24 * 2**20
        ),
        cost_estimate=pl.CostEstimate(
            flops=20_000_000_000, bytes_accessed=20_000_000, transcendentals=8_000_000
        ),
        name="attention",
    )(qkv, qkv, qkv, rank_rows, second, bias[None, :], surge.T[:, :, None], gain[None, :])


def on_device(
    n_rep,
    n_tp,
    tokens,
    attention_pre_gain,
    query_matrix,
    key_matrix,
    value_matrix,
    decay_first_weight,
    decay_second_weight,
    decay_offset_bias,
    extra_log_surge,
    readout_head_gain,
    output_matrix,
    attention_post_gain,
    feedforward_pre_gain,
    up_matrix,
    down_matrix,
    feedforward_post_gain,
):
    me = lax.axis_index("tp")
    rep = lax.axis_index("rep")
    swap = [(i, 1 - i) for i in range(2)]

    def both_halves(mine):
        if n_tp != 2:
            return lax.all_gather(mine, "tp", axis=1, tiled=True)
        other = lax.ppermute(mine, "tp", swap)
        first = me == 0
        return jnp.concatenate(
            [jnp.where(first, mine, other), jnp.where(first, other, mine)], axis=1
        )

    def sum_scattered(partial):
        if n_tp != 2:
            return lax.psum_scatter(partial, "tp", scatter_dimension=1, tiled=True).astype(
                jnp.float32
            )
        size = partial.shape[1] // 2
        keep = lax.dynamic_slice_in_dim(partial, me * size, size, 1)
        send = lax.dynamic_slice_in_dim(partial, (1 - me) * size, size, 1)
        return keep.astype(jnp.float32) + lax.ppermute(send, "tp", swap).astype(jnp.float32)

    def summed(rows):
        if n_tp != 2:
            return lax.psum(rows, "tp")
        return rows + lax.ppermute(rows, "tp", swap)

    def part(weight, axis):
        size = weight.shape[axis] // n_rep
        return lax.dynamic_slice_in_dim(weight, rep * size, size, axis)

    weights = jnp.concatenate([query_matrix, key_matrix, value_matrix], axis=1)
    with jax.named_scope("gather_in"):
        whole_in = lax.all_gather(weights, "fs", axis=0, tiled=True)
    with jax.named_scope("gather_out"):
        whole_out = lax.all_gather(output_matrix, "fs", axis=1, tiled=True)
    with jax.named_scope("gather_up"):
        whole_up = lax.all_gather(part(up_matrix, 1), ("rep", "fs"), axis=0, tiled=True)
    with jax.named_scope("gather_down"):
        whole_down = lax.all_gather(part(down_matrix, 0), ("rep", "fs"), axis=1, tiled=True)

    gathered = both_halves(tokens)
    width = gathered.shape[1]
    normed = pre_norm(gathered, attention_pre_gain)
    rank_rows = jnp.dot(normed, decay_first_weight, preferred_element_type=jnp.float32).astype(
        jnp.bfloat16
    )
    with jax.named_scope("project"):
        qkv = jnp.dot(normed, whole_in, preferred_element_type=jnp.float32).astype(jnp.bfloat16)
    with jax.named_scope("mix"):
        mixed = attention(
            qkv, rank_rows, decay_second_weight, decay_offset_bias, extra_log_surge,
            readout_head_gain,
        )
    with jax.named_scope("out_project"):
        partial_attn = jnp.dot(mixed, whole_out, preferred_element_type=jnp.float32)
    attn = sum_scattered(partial_attn.astype(jnp.bfloat16))
    attn_total = summed(jnp.sum(attn * attn, axis=1))
    attn_scale = lax.rsqrt(attn_total / width + EPS)[:, None]
    resid = (tokens.astype(jnp.float32) + attn * attn_scale * attention_post_gain).astype(
        jnp.bfloat16
    )
    normed_mid = pre_norm(both_halves(resid), feedforward_pre_gain)
    up_parts = whole_up.reshape(n_rep, width, -1)
    squared = []
    for r in range(n_rep):
        hidden = jax.nn.relu(
            jnp.dot(normed_mid, up_parts[r], preferred_element_type=jnp.float32)
        )
        squared.append((hidden * hidden).astype(jnp.bfloat16))
    partial_feed = sum(
        jnp.dot(
            squared[r],
            whole_down[:, r * width : (r + 1) * width],
            preferred_element_type=jnp.float32,
        )
        for r in range(n_rep)
    )
    feed = sum_scattered(partial_feed.astype(jnp.bfloat16))
    feed_total = summed(jnp.sum(feed * feed, axis=1))
    feed_scale = lax.rsqrt(feed_total / width + EPS)[:, None]
    return (resid.astype(jnp.float32) + feed * feed_scale * feedforward_post_gain).astype(
        jnp.bfloat16
    )


def solution(mesh):
    return jax.shard_map(
        functools.partial(on_device, mesh.shape["rep"], mesh.shape["tp"]),
        mesh=mesh,
        in_specs=(
            P(("rep", "fs"), "tp"),
            P(),
            P("fs", "tp"),
            P("fs", "tp"),
            P("fs", "tp"),
            P(),
            P(None, "tp"),
            P("tp"),
            P(("rep", "fs"), "tp"),
            P(),
            P("tp", "fs"),
            P("tp"),
            P(),
            P("fs", "tp"),
            P("tp", "fs"),
            P("tp"),
        ),
        out_specs=P(("rep", "fs"), "tp"),
        check_vma=False,
    )
```

```python
import functools

import jax
import jax.numpy as jnp
from jax import lax
from jax.experimental import pallas as pl
from jax.experimental.pallas import tpu as pltpu
from jax.sharding import PartitionSpec as P

KEY_WIDTH = 256
DV = 512
LENGTH = 1024
CHUNK = 128
SUB = 16
EPS = 1e-06


def pre_norm(rows, gain):
    values = rows.astype(jnp.float32)
    scale = lax.rsqrt(jnp.mean(values * values, axis=-1, keepdims=True) + EPS)
    return (values * scale * gain).astype(jnp.bfloat16)


def attention_kernel(
    q_ref, k_ref, v_ref, rank_ref, second_ref, bias_ref, surge_ref, gain_ref, o_ref, state
):
    subs = CHUNK // SUB

    @pl.when(lax.rem(pl.program_id(1), LENGTH // CHUNK) == 0)
    def _():
        state[...] = jnp.zeros_like(state)

    q = q_ref[...].astype(jnp.float32) * KEY_WIDTH ** (-0.5)
    k = k_ref[...].astype(jnp.float32)
    v = v_ref[...]
    source = (
        jnp.dot(rank_ref[...], second_ref[...], preferred_element_type=jnp.float32)
        + bias_ref[...]
    )
    log_sig = jnp.minimum(source, 0.0) - jnp.log1p(jnp.exp(-jnp.abs(source)))
    gate = log_sig / 16.0 + surge_ref[0]

    row = lax.broadcasted_iota(jnp.int32, (CHUNK, CHUNK), 0)
    col = lax.broadcasted_iota(jnp.int32, (CHUNK, CHUNK), 1)
    lower = (row >= col).astype(jnp.float32)
    cum = jnp.dot(
        lower, gate, preferred_element_type=jnp.float32, precision=lax.Precision.HIGHEST
    )

    q3 = q.reshape(subs, SUB, KEY_WIDTH)
    k3 = k.reshape(subs, SUB, KEY_WIDTH)
    c3 = cum.reshape(subs, SUB, KEY_WIDTH)
    pick_col = lax.rem(lax.broadcasted_iota(jnp.int32, (KEY_WIDTH, CHUNK), 1), SUB)
    scores = jnp.zeros((CHUNK, CHUNK), jnp.float32)
    for j in range(SUB):
        weight = jnp.exp(jnp.minimum(c3 - c3[:, j : j + 1, :], 0.0))
        term = (q3 * k3[:, j : j + 1, :] * weight).reshape(CHUNK, KEY_WIDTH)
        scores += jnp.dot(
            term.astype(jnp.bfloat16),
            (pick_col == j).astype(jnp.bfloat16),
            preferred_element_type=jnp.float32,
        )
    scores = jnp.where((row // SUB == col // SUB) & (row >= col), scores, 0.0)

    pieces = [jnp.zeros((SUB, CHUNK), jnp.float32)]
    key_row = lax.broadcasted_iota(jnp.int32, (CHUNK, KEY_WIDTH), 0)
    for i in range(1, subs):
        edge = cum[i * SUB - 1 : i * SUB, :]
        left = q3[i] * jnp.exp(jnp.minimum(c3[i] - edge, 0.0))
        right = jnp.where(key_row < i * SUB, k * jnp.exp(jnp.minimum(edge - cum, 0.0)), 0.0)
        pieces.append(
            lax.dot_general(
                left.astype(jnp.bfloat16),
                right.astype(jnp.bfloat16),
                (((1,), (1,)), ((), ())),
                preferred_element_type=jnp.float32,
            )
        )
    scores = scores + jnp.concatenate(pieces, axis=0)

    last = cum[CHUNK - 1 : CHUNK, :]
    held = state[...]
    readout = lax.dot_general(
        (q * jnp.exp(cum)).astype(jnp.bfloat16),
        held.astype(jnp.bfloat16),
        (((1,), (1,)), ((), ())),
        preferred_element_type=jnp.float32,
    ) + jnp.dot(scores.astype(jnp.bfloat16), v, preferred_element_type=jnp.float32)
    faded = (k * jnp.exp(jnp.minimum(last - cum, 0.0))).astype(jnp.bfloat16)
    state[...] = held * jnp.exp(last) + lax.dot_general(
        v, faded, (((0,), (0,)), ((), ())), preferred_element_type=jnp.float32
    )
    scale = lax.rsqrt(jnp.mean(readout * readout, axis=-1, keepdims=True) + EPS)
    o_ref[...] = (readout * scale * gain_ref[...]).astype(jnp.bfloat16)


def attention(qkv, rank_rows, second, bias, surge, gain):
    tokens = qkv.shape[0]
    heads = second.shape[1] // KEY_WIDTH
    rank = rank_rows.shape[1]
    value_base = 2 * heads * KEY_WIDTH // DV
    return pl.pallas_call(
        attention_kernel,
        grid=(heads, tokens // CHUNK),
        in_specs=[
            pl.BlockSpec((CHUNK, KEY_WIDTH), lambda h, c: (c, h)),
            pl.BlockSpec((CHUNK, KEY_WIDTH), lambda h, c: (c, heads + h)),
            pl.BlockSpec((CHUNK, DV), lambda h, c: (c, value_base + h)),
            pl.BlockSpec((CHUNK, rank), lambda h, c: (c, 0)),
            pl.BlockSpec((rank, KEY_WIDTH), lambda h, c: (0, h)),
            pl.BlockSpec((1, KEY_WIDTH), lambda h, c: (0, h)),
            pl.BlockSpec((1, CHUNK, 1), lambda h, c: (h, c, 0)),
            pl.BlockSpec((1, DV), lambda h, c: (0, 0)),
        ],
        out_specs=pl.BlockSpec((CHUNK, DV), lambda h, c: (c, h)),
        out_shape=jax.ShapeDtypeStruct((tokens, heads * DV), jnp.bfloat16),
        scratch_shapes=[pltpu.VMEM((DV, KEY_WIDTH), jnp.float32)],
        compiler_params=pltpu.CompilerParams(
            dimension_semantics=("arbitrary", "arbitrary"), vmem_limit_bytes=24 * 2**20
        ),
        cost_estimate=pl.CostEstimate(
            flops=20_000_000_000, bytes_accessed=20_000_000, transcendentals=8_000_000
        ),
        name="attention",
    )(qkv, qkv, qkv, rank_rows, second, bias[None, :], surge.T[:, :, None], gain[None, :])


def on_device(
    n_rep,
    n_fs,
    n_tp,
    tokens,
    attention_pre_gain,
    query_matrix,
    key_matrix,
    value_matrix,
    decay_first_weight,
    decay_second_weight,
    decay_offset_bias,
    extra_log_surge,
    readout_head_gain,
    output_matrix,
    attention_post_gain,
    feedforward_pre_gain,
    up_matrix,
    down_matrix,
    feedforward_post_gain,
):
    me = lax.axis_index("tp")
    rep = lax.axis_index("rep")
    swap = [(i, 1 - i) for i in range(2)]

    def both_halves(mine):
        if n_tp != 2:
            return lax.all_gather(mine, "tp", axis=1, tiled=True)
        other = lax.ppermute(mine, "tp", swap)
        first = me == 0
        return jnp.concatenate(
            [jnp.where(first, mine, other), jnp.where(first, other, mine)], axis=1
        )

    def sum_scattered(partial):
        if n_tp != 2:
            return lax.psum_scatter(partial, "tp", scatter_dimension=1, tiled=True).astype(
                jnp.float32
            )
        size = partial.shape[1] // 2
        keep = lax.dynamic_slice_in_dim(partial, me * size, size, 1)
        send = lax.dynamic_slice_in_dim(partial, (1 - me) * size, size, 1)
        return keep.astype(jnp.float32) + lax.ppermute(send, "tp", swap).astype(jnp.float32)

    def summed(rows):
        if n_tp != 2:
            return lax.psum(rows, "tp")
        return rows + lax.ppermute(rows, "tp", swap)

    def part(weight, axis):
        size = weight.shape[axis] // n_rep
        return lax.dynamic_slice_in_dim(weight, rep * size, size, axis)

    weights = jnp.concatenate([query_matrix, key_matrix, value_matrix], axis=1)
    with jax.named_scope("gather_in"):
        whole_in = lax.all_gather(weights, "fs", axis=0, tiled=True)
    with jax.named_scope("gather_out"):
        whole_out = lax.all_gather(output_matrix, "fs", axis=1, tiled=True)
    rows = up_matrix.shape[0]
    cols = down_matrix.shape[1]
    mine = lax.axis_index("fs")
    place = jnp.where(mine % 2 == 0, mine // 2, n_fs - 1 - mine // 2)
    cycle = [2 * p if p < n_fs // 2 else 2 * (n_fs - 1 - p) + 1 for p in range(n_fs)]
    ahead = [(cycle[p], cycle[(p + 1) % n_fs]) for p in range(n_fs)]
    behind = [(to, at) for at, to in ahead]

    def shard_at(p):
        p = (p + n_fs) % n_fs
        return jnp.where(p < n_fs // 2, 2 * p, 2 * (n_fs - 1 - p) + 1)

    def travel(own, hops_ahead, hops_behind):
        chunks = []
        for hops, ring, sign in ((hops_ahead, ahead, -1), (hops_behind, behind, 1)):
            piece = own
            for step in range(1, hops + 1):
                piece = lax.ppermute(piece, "fs", ring)
                chunks.append((step, shard_at(place + sign * step), piece))
        chunks.sort(key=lambda c: c[0])
        pieces = [(piece, rep, shard) for _, shard, piece in chunks]
        others = []
        for piece, _, shard in pieces:
            for turn in range(1, n_rep):
                other = lax.ppermute(
                    piece, "rep", [(r, (r + turn) % n_rep) for r in range(n_rep)]
                )
                others.append((other, (rep + n_rep - turn) % n_rep, shard))
        return pieces, others

    def hold_until(value, moved):
        tied = lax.optimization_barrier((value, *[m[0] for m in moved]))
        return tied[0], [(t, *m[1:]) for t, m in zip(tied[1:], moved)]

    up_cols = up_matrix.shape[1] // n_rep
    down_rows = down_matrix.shape[0] // n_rep
    half = n_fs // 2
    up_pieces, up_others = travel(part(up_matrix, 1), half, n_fs - 1 - half)
    with jax.named_scope("gather_down"):
        whole_down = lax.all_gather(down_matrix, "fs", axis=1, tiled=True)

    gathered = both_halves(tokens)
    width = gathered.shape[1]
    normed = pre_norm(gathered, attention_pre_gain)
    rank_rows = jnp.dot(normed, decay_first_weight, preferred_element_type=jnp.float32).astype(
        jnp.bfloat16
    )
    early = up_pieces + up_others[: half]
    normed, early = hold_until(normed, early)
    with jax.named_scope("project"):
        qkv = jnp.dot(normed, whole_in, preferred_element_type=jnp.float32).astype(jnp.bfloat16)
    with jax.named_scope("mix"):
        mixed = attention(
            qkv, rank_rows, decay_second_weight, decay_offset_bias, extra_log_surge,
            readout_head_gain,
        )
    mixed, late = hold_until(mixed, up_others[half :])
    with jax.named_scope("out_project"):
        partial_attn = jnp.dot(mixed, whole_out, preferred_element_type=jnp.float32)
    attn = sum_scattered(partial_attn.astype(jnp.bfloat16))
    attn_total = summed(jnp.sum(attn * attn, axis=1))
    attn_scale = lax.rsqrt(attn_total / width + EPS)[:, None]
    resid = (tokens.astype(jnp.float32) + attn * attn_scale * attention_post_gain).astype(
        jnp.bfloat16
    )
    normed_mid = pre_norm(both_halves(resid), feedforward_pre_gain)
    whole_up = lax.dynamic_update_slice(
        jnp.zeros((n_fs * rows, up_matrix.shape[1]), jnp.bfloat16), up_matrix, (mine * rows, 0)
    )
    for piece, r, j in early + late:
        whole_up = lax.dynamic_update_slice(whole_up, piece, (j * rows, r * up_cols))
    hidden = jax.nn.relu(jnp.dot(normed_mid, whole_up, preferred_element_type=jnp.float32))
    squared = (hidden * hidden).astype(jnp.bfloat16)
    partial_feed = jnp.dot(squared, whole_down, preferred_element_type=jnp.float32)
    feed = sum_scattered(partial_feed.astype(jnp.bfloat16))
    feed_total = summed(jnp.sum(feed * feed, axis=1))
    feed_scale = lax.rsqrt(feed_total / width + EPS)[:, None]
    return (resid.astype(jnp.float32) + feed * feed_scale * feedforward_post_gain).astype(
        jnp.bfloat16
    )


def solution(mesh):
    return jax.shard_map(
        functools.partial(on_device, mesh.shape["rep"], mesh.shape["fs"], mesh.shape["tp"]),
        mesh=mesh,
        in_specs=(
            P(("rep", "fs"), "tp"),
            P(),
            P("fs", "tp"),
            P("fs", "tp"),
            P("fs", "tp"),
            P(),
            P(None, "tp"),
            P("tp"),
            P(("rep", "fs"), "tp"),
            P(),
            P("tp", "fs"),
            P("tp"),
            P(),
            P("fs", "tp"),
            P("tp", "fs"),
            P("tp"),
        ),
        out_specs=P(("rep", "fs"), "tp"),
        check_vma=False,
    )
```
